32 devices in a mesh: fs: 8 (over z, y), tp: 4 (over x, core).
Axes of the slice: x: 2, y: 2, z: 4, core: 2. Of those that a mesh axis runs over, the one named last changes fastest.
Arguments:
- stream: bfloat16 [3072, 2048], P('fs', 'tp'), may hold values from -3 to 3
- gain_first: float32 [2048], replicated, may hold values from 0.1 to 1.9
- gain_mixer: float32 [2048], replicated, may hold values from 0.1 to 1.9
- gain_second: float32 [2048], replicated, may hold values from 0.1 to 1.9
- gate_weight: float32 [2048, 5632], P('fs', 'tp'), may hold values from -0.125 to 0.125
- gate_scale: float32 [5632], P('tp'), may hold values from 0.5 to 2
- up_weight: float32 [2048, 5632], P('fs', 'tp'), may hold values from -0.125 to 0.125
- up_scale: float32 [5632], P('tp'), may hold values from 0.5 to 2
- down_weight: float32 [5632, 2048], P('tp', 'fs'), may hold values from -0.109375 to 0.109375
- down_scale: float32 [2048], P('tp'), may hold values from 0.5 to 2
- pool_in_weight: float32 [2048, 512], P('fs', 'tp'), may hold values from -0.125 to 0.125
- pool_in_scale: float32 [512], P('tp'), may hold values from 0.5 to 2
- pool_out_weight: float32 [512, 2048], P('tp', 'fs'), may hold values from -0.375 to 0.375
- pool_out_scale: float32 [2048], P('tp'), may hold values from 0.5 to 2
Outputs:
- layer_out: bfloat16 [3072, 2048], P('fs', 'tp')
The draws below stay inside these ranges and needn't reach their ends.
All inputs are finite; a program needn't handle non-finite values.
Results may differ from the reference program's by a relative error of at most 0.025.
Values may be sent and summed in bfloat16 or wider, within the bound.
A program may use at most 64 MiB of HBM per device.

```python
import math
import jax
import jax.numpy as jnp
from jax import lax

D = 2048
FF = 5632
P_SIZE = 512
SEQ = 128
TOKENS = 3072
N_TP = 4


def strengthened(drawn, rng, source, target, blocks, factor):
    owner, partner = [(jnp.arange(drawn.shape[dim]) // (drawn.shape[dim] // blocks)).reshape([-1 if axis == dim else 1 for axis in range(drawn.ndim)]) for dim in (source, target)]
    chosen = jax.random.permutation(rng, blocks)[partner]
    strong = (owner == chosen) | (owner == (partner + blocks // 2) % blocks)
    return jnp.where(strong, factor * drawn, drawn)


def level_of(stream_key, extent, cuts, least, top_value):
    level, own = 1.0, jax.random.fold_in(stream_key, 6)
    for axis_at, blocks in cuts:
        steps = jnp.exp(jax.random.uniform(jax.random.fold_in(own, axis_at), (blocks,), jnp.float32, least / len(cuts), top_value / len(cuts)))
        level = level * jnp.repeat(steps, extent[axis_at] // blocks).reshape([-1 if axis == axis_at else 1 for axis in range(len(extent))])
    return level


def normal_values(own_key, extent, scale, limit, cuts=(), kind=jnp.bfloat16):
    values = jax.random.normal(own_key, extent, jnp.float32) * scale
    if len(cuts) > 0:
        values = level_of(own_key, extent, cuts, -0.22, 0.18) * values
    return jnp.clip(values, min=-limit, max=limit).astype(kind)


def heavy_noise(key, shape, width, bound, pieces, heavy, dtype=jnp.bfloat16):
    result = width * jax.random.normal(key, shape, jnp.float32)
    if pieces:
        result = result * level_of(key, shape, pieces, -0.22, 0.18)
    return jnp.clip(strengthened(result, jax.random.fold_in(key, 3), *heavy), -bound, bound).astype(dtype)


def setup_inputs(seed: int = 0) -> dict:
    streams_of = jax.random.split(jax.random.key(seed), 15)
    return {
        "stream": normal_values(streams_of[0], (TOKENS, D), 0.5, 3.0, ((0, 8), (1, 4))),
        "gain_first": jnp.clip(1.0 + 0.18 * jax.random.normal(streams_of[1], (D,), jnp.float32), 0.1, 1.9),
        "gain_mixer": jnp.clip(1.0 + 0.18 * jax.random.normal(streams_of[2], (D,), jnp.float32), 0.1, 1.9),
        "gain_second": jnp.clip(1.0 + 0.18 * jax.random.normal(streams_of[3], (D,), jnp.float32), 0.1, 1.9),
        "gate_weight": normal_values(streams_of[4], (D, FF), D ** -0.5, 0.125, ((0, 8), (1, 4)), jnp.float32),
        "gate_scale": jnp.clip(jnp.exp(math.log(2.0) - 1.3862944 * jax.random.uniform(streams_of[5], (FF,), jnp.float32) ** level_of(streams_of[5], (FF,), ((0, 4),), -0.2, 0.2)), 0.5, 2.0),
        "up_weight": normal_values(streams_of[6], (D, FF), D ** -0.5, 0.125, ((0, 8), (1, 4)), jnp.float32),
        "up_scale": jnp.clip(jnp.exp(math.log(2.0) - 1.3862944 * jax.random.uniform(streams_of[7], (FF,), jnp.float32) ** level_of(streams_of[7], (FF,), ((0, 4),), -0.2, 0.2)), 0.5, 2.0),
        "down_weight": heavy_noise(streams_of[8], (FF, D), FF ** -0.5, 0.109375, ((0, 4), (1, 8)), (0, 1, 8, 2.0), jnp.float32),
        "down_scale": jnp.clip(jnp.exp(math.log(2.0) - 1.3862944 * jax.random.uniform(streams_of[9], (D,), jnp.float32) ** level_of(streams_of[9], (D,), ((0, 4),), -0.2, 0.2)), 0.5, 2.0),
        "pool_in_weight": normal_values(streams_of[10], (D, P_SIZE), D ** -0.5, 0.125, ((0, 8), (1, 4)), jnp.float32),
        "pool_in_scale": jnp.clip(jnp.exp(math.log(2.0) - 1.3862944 * jax.random.uniform(streams_of[11], (P_SIZE,), jnp.float32) ** level_of(streams_of[11], (P_SIZE,), ((0, 4),), -0.2, 0.2)), 0.5, 2.0),
        "pool_out_weight": heavy_noise(streams_of[12], (P_SIZE, D), P_SIZE ** -0.5, 0.375, ((0, 4), (1, 8)), (0, 1, 8, 2.0), jnp.float32),
        "pool_out_scale": jnp.clip(jnp.exp(math.log(2.0) - 1.3862944 * jax.random.uniform(streams_of[13], (D,), jnp.float32) ** level_of(streams_of[13], (D,), ((0, 4),), -0.2, 0.2)), 0.5, 2.0),
    }


eps = 1e-06
WINDOWS = (2, 4, 8, 16)

def rms_norm(values, norm_gain):
    floats = values.astype(jnp.float32)
    scaled = floats * lax.rsqrt(lax.optimization_barrier(jnp.mean(floats * floats, axis=-1, keepdims=True)) + eps)
    return (scaled * norm_gain).astype(jnp.bfloat16)

def block_sum(left_rows, right_rows, column_scale):
    block_rows = right_rows.shape[0] // N_TP
    running = jnp.zeros((left_rows.shape[0], right_rows.shape[1]), jnp.float32)
    for blocks in range(N_TP):
        block_part = jnp.dot(left_rows[:, blocks * block_rows:(blocks + 1) * block_rows], right_rows[blocks * block_rows:(blocks + 1) * block_rows], preferred_element_type=jnp.float32).astype(jnp.bfloat16)
        block_part = lax.optimization_barrier(block_part)
        running = running + block_part.astype(jnp.float32)
    return running * column_scale

def feed_forward(normed, gate_half, gate_scale, up_half, up_scale, down_half, down_scale):
    gate_sum = jnp.dot(normed, gate_half, preferred_element_type=jnp.float32) * gate_scale
    up_sum = jnp.dot(normed, up_half, preferred_element_type=jnp.float32) * up_scale
    hidden = (jax.nn.silu(gate_sum) * up_sum).astype(jnp.bfloat16)
    return block_sum(hidden, down_half, down_scale)

def pooling(pool_input):
    channels = pool_input.shape[1]
    floats = pool_input.astype(jnp.float32).reshape(-1, SEQ, channels)
    csum = jnp.concatenate([jnp.zeros((floats.shape[0], 1, channels), jnp.float32), jnp.cumsum(floats, axis=1)], axis=1)
    position = jnp.arange(SEQ)
    channel_group = jnp.arange(channels) * 4 // channels
    pooled = -floats
    for group_index, window in enumerate(WINDOWS):
        before = window // 2
        after_span = window - before
        upper_sum = jnp.pad(csum, ((0, 0), (0, after_span), (0, 0)), mode='edge')[:, after_span:after_span + SEQ]
        lower_sum = jnp.pad(csum, ((0, 0), (before, 0), (0, 0)), mode='edge')[:, :SEQ]
        counts = (jnp.minimum(position + after_span, SEQ) - jnp.maximum(position - before, 0)).astype(jnp.float32)
        window_mean = (upper_sum - lower_sum) / counts[None, :, None]
        select = (channel_group == group_index).astype(jnp.float32)
        pooled = pooled + window_mean * select
    return pooled.reshape(-1, channels).astype(jnp.bfloat16)

def reference(stream, gain_first, gain_mixer, gain_second, gate_weight, gate_scale, up_weight, up_scale, down_weight, down_scale, pool_in_weight, pool_in_scale, pool_out_weight, pool_out_scale):
    gate_half = gate_weight.astype(jnp.bfloat16)
    up_half = up_weight.astype(jnp.bfloat16)
    down_half = down_weight.astype(jnp.bfloat16)
    in_half = pool_in_weight.astype(jnp.bfloat16)
    out_half = pool_out_weight.astype(jnp.bfloat16)
    first_branch = feed_forward(rms_norm(stream, gain_first), gate_half, gate_scale, up_half, up_scale, down_half, down_scale)
    after_first = (stream.astype(jnp.float32) + 0.5 * first_branch).astype(jnp.bfloat16)
    mixer_normed = rms_norm(after_first, gain_mixer)
    pool_input = (jnp.dot(mixer_normed, in_half, preferred_element_type=jnp.float32) * pool_in_scale).astype(jnp.bfloat16)
    pooled = pooling(pool_input)
    after_mix = (after_first.astype(jnp.float32) + block_sum(pooled, out_half, pool_out_scale)).astype(jnp.bfloat16)
    second_branch = feed_forward(rms_norm(after_mix, gain_second), gate_half, gate_scale, up_half, up_scale, down_half, down_scale)
    return (after_mix.astype(jnp.float32) + 0.5 * second_branch).astype(jnp.bfloat16)
```

```python
import functools

import jax
import jax.numpy as jnp
from jax import lax
from jax.experimental import pallas as pl
from jax.experimental.pallas import tpu as pltpu
from jax.sharding import PartitionSpec as P

SEQ = 128
MESH = pl.DeviceIdType.MESH

eps = 1e-06
WINDOWS = (2, 4, 8, 16)


def fs_grid(count):
    ny = 1
    while (2 * ny) * (2 * ny) <= count and count % (2 * ny) == 0:
        ny *= 2
    return ny, count // ny


def gather_kernel(nfs, ntp, pool, gate, up, down, stream, pool_all, gate_all, up_all, down_all, stream_all,
                  send_sem, recv_sem, local_sem, tsend, trecv, psend, precv):
    ny, nz = fs_grid(nfs)
    nx = ntp // 2
    fs, tp = lax.axis_index("fs"), lax.axis_index("tp")
    z, y = fs // ny, fs % ny
    x, core = tp // 2, tp % 2
    partner = x * 2 + (1 - core)
    alternate = ny == 2 and nz > 1

    barrier = pltpu.get_barrier_semaphore()

    def greet(cond, f, t):
        @pl.when(cond)
        def _():
            pl.semaphore_signal(barrier, inc=1, device_id={"fs": f, "tp": t}, device_id_type=MESH)

    greet(z > 0, fs - ny, tp)
    greet(z < nz - 1, fs + ny, tp)
    greet(y > 0, fs - 1, tp)
    greet(y < ny - 1, fs + 1, tp)
    pl.semaphore_signal(barrier, inc=1, device_id={"fs": fs, "tp": partner}, device_id_type=MESH)
    for k in range(1, nx):
        pl.semaphore_signal(
            barrier, inc=1, device_id={"fs": fs, "tp": (x + k) % nx * 2 + core}, device_id_type=MESH
        )
    peers = nx
    for cond in (z > 0, z < nz - 1, y > 0, y < ny - 1):
        peers = peers + jnp.where(cond, 1, 0)
    pl.semaphore_wait(barrier, peers)

    pieces = [(lambda: pool, lambda f: pool_all.at[tp, f])]
    for own, whole in ((gate, gate_all), (up, up_all), (down, down_all)):
        rows = own.shape[0]
        halves = 2 if alternate else 1
        for h in range(halves):
            part = pl.ds(h * (rows // halves), rows // halves)
            pieces.append((
                functools.partial(lambda own, part: own.at[part], own, part),
                functools.partial(lambda whole, part, f: whole.at[f, part], whole, part),
            ))
    started = []

    def remote(piece, f, direction, target, mine=False):
        own, whole = pieces[piece]
        return pltpu.make_async_remote_copy(
            src_ref=own() if mine else whole(f),
            dst_ref=whole(f),
            send_sem=send_sem.at[piece, f, direction],
            recv_sem=recv_sem.at[piece, f],
            device_id={"fs": target, "tp": tp},
            device_id_type=MESH,
        )

    def send(cond, piece, f, direction, mine=False):
        target = fs + (-ny, ny, -1, 1)[direction]

        @pl.when(cond)
        def _():
            remote(piece, f, direction, target, mine).start()

        started.append((cond, piece, f, direction, target, mine))

    def arrived(cond, piece, f):
        @pl.when(cond)
        def _():
            remote(piece, f, 0, fs, False).wait_recv()

    def by_y(cond, piece, f, mine=False):
        send(cond & (y > 0), piece, f, 2, mine)
        send(cond & (y < ny - 1), piece, f, 3, mine)

    yes = z >= 0

    def stream_copy(src, slot, t_target, k):
        return pltpu.make_async_remote_copy(
            src_ref=src, dst_ref=stream_all.at[slot], send_sem=tsend.at[k], recv_sem=trecv.at[slot],
            device_id={"fs": fs, "tp": t_target}, device_id_type=MESH)

    def pool_copy(slot, t_target, k):
        return pltpu.make_async_remote_copy(
            src_ref=pool_all.at[slot], dst_ref=pool_all.at[slot], send_sem=psend.at[k], recv_sem=precv.at[slot],
            device_id={"fs": fs, "tp": t_target}, device_id_type=MESH)

    npieces = len(pieces)
    locals_ = [pltpu.make_async_copy(own(), whole(fs), local_sem.at[i]) for i, (own, whole) in enumerate(pieces)]
    locals_.append(pltpu.make_async_copy(stream, stream_all.at[tp], local_sem.at[npieces]))
    for piece in range(npieces):
        send(z > 0, piece, fs, 0, True)
        send(z < nz - 1, piece, fs, 1, True)
        by_y(yes, piece, fs, True)
    stream_sends = []
    for k in range(1, nx):
        stream_sends.append(stream_copy(stream, tp, (x + k) % nx * 2 + core, k - 1))
    stream_sends.append(stream_copy(stream, tp, partner, nx - 1))
    for copy in stream_sends:
        copy.start()
    for copy in locals_:
        copy.start()

    def row_arrivals(piece, d, alt):
        low, high = fs - d * ny, fs + d * ny
        has_low, has_high = z >= d, z + d <= nz - 1
        for cond, f, direction, ahead, end in (
            (has_low, low, 1, z < nz - 1, z == d),
            (has_high, high, 0, z > 0, z + d == nz - 1),
        ):
            arrived(cond, piece, f)
            send(cond & ahead, piece, f, direction)
            if alt:
                by_y(cond & jnp.logical_not(end), piece, f)
                other = f + 1 - 2 * y
                arrived(cond & end, piece, other)
                send(cond & end & ahead, piece, other, direction)
            else:
                by_y(cond, piece, f)

    def column_arrivals(piece, alt):
        for d in range(nz):
            for sign in ((1,) if d == 0 else (-1, 1)):
                row_ok = (z + sign * d >= 0) & (z + sign * d <= nz - 1)
                if alt:
                    at = z + sign * d
                    if d == 0:
                        continue
                    row_ok = row_ok & (at != 0) & (at != nz - 1)
                base = fs + sign * d * ny
                for e in range(1, ny):
                    for step, direction, ok, ahead in (
                        (-e, 3, y >= e, y < ny - 1),
                        (e, 2, y + e <= ny - 1, y > 0),
                    ):
                        arrived(row_ok & ok, piece, base + step)
                        if ny > 2:
                            send(row_ok & ok & ahead, piece, base + step, direction)

    is_alt = [alternate and p > 0 and p % 2 == 0 for p in range(npieces)]

    for d in range(1, nz):
        row_arrivals(0, d, False)
    column_arrivals(0, False)
    locals_[0].wait()
    pool_sends = [pool_copy(tp, (x + k) % nx * 2 + core, k - 1) for k in range(1, nx)]
    pool_sends.append(pool_copy(tp, partner, nx - 1))
    for copy in pool_sends:
        copy.start()
    for k in range(1, nx):
        slot = (x + k) % nx * 2 + core
        stream_copy(stream, slot, partner, 0).wait_recv()
        copy = stream_copy(stream_all.at[slot], slot, partner, nx - 1 + k)
        copy.start()
        stream_sends.append(copy)

    for p in range(npieces):
        if is_alt[p]:
            other = fs + 1 - 2 * y
            arrived(yes, p, other)
            send(z == 0, p, other, 1)
            send(z == nz - 1, p, other, 0)
    for d in range(1, nz):
        for p in range(1, npieces):
            row_arrivals(p, d, is_alt[p])
        if d == 1:
            for k in range(1, nx):
                slot = (x + k) % nx * 2 + core
                pool_copy(slot, partner, 0).wait_recv()
                copy = pool_copy(slot, partner, nx - 1 + k)
                copy.start()
                pool_sends.append(copy)
    for p in range(1, npieces):
        column_arrivals(p, is_alt[p])
    for k in range(nx):
        slot = (x + k) % nx * 2 + (1 - core)
        stream_copy(stream, slot, partner, 0).wait_recv()
        pool_copy(slot, partner, 0).wait_recv()
    for copy in locals_[1:]:
        copy.wait()
    for copy in stream_sends + pool_sends:
        copy.wait_send()
    for cond, piece, f, direction, target, mine in started:
        @pl.when(cond)
        def _():
            remote(piece, f, direction, target, mine).wait_send()


def gather_all(nfs, ntp, pool, gate, up, down, stream):
    ny, nz = fs_grid(nfs)
    nx = ntp // 2
    npieces = 7 if (ny == 2 and nz > 1) else 4
    dtype = jnp.bfloat16
    any_spec = pl.BlockSpec(memory_space=pl.ANY)
    return pl.pallas_call(
        functools.partial(gather_kernel, nfs, ntp),
        name="collect_weights",
        out_shape=(
            jax.ShapeDtypeStruct((ntp, nfs) + pool.shape, dtype),
            jax.ShapeDtypeStruct((nfs,) + gate.shape, dtype),
            jax.ShapeDtypeStruct((nfs,) + up.shape, dtype),
            jax.ShapeDtypeStruct((nfs,) + down.shape, dtype),
            jax.ShapeDtypeStruct((ntp,) + stream.shape, dtype),
        ),
        in_specs=[any_spec] * 5,
        out_specs=[any_spec] * 5,
        scratch_shapes=[
            pltpu.SemaphoreType.DMA((npieces, nfs, 4)),
            pltpu.SemaphoreType.DMA((npieces, nfs)),
            pltpu.SemaphoreType.DMA((npieces + 1,)),
            pltpu.SemaphoreType.DMA((2 * nx,)),
            pltpu.SemaphoreType.DMA((ntp,)),
            pltpu.SemaphoreType.DMA((2 * nx,)),
            pltpu.SemaphoreType.DMA((ntp,)),
        ],
        compiler_params=pltpu.CompilerParams(collective_id=0, has_side_effects=True, vmem_limit_bytes=1 << 20),
    )(pool, gate, up, down, stream)


def sum_kernel(ntp, gathers, pieces, partial, resid, scale, out, pair, pair_sum, cross, *sems):
    pair_send, pair_recv, cross_send, cross_recv = sems[:4]
    nx = ntp // 2
    tp, fs = lax.axis_index("tp"), lax.axis_index("fs")
    x, core = tp // 2, tp % 2
    partner = x * 2 + (1 - core)
    rows, width = resid.shape
    step = rows // pieces
    barrier = pltpu.get_barrier_semaphore()
    pl.semaphore_signal(barrier, inc=1, device_id={"fs": fs, "tp": partner}, device_id_type=MESH)
    for k in range(1, nx):
        pl.semaphore_signal(
            barrier, inc=1, device_id={"fs": fs, "tp": (x + k) % nx * 2 + core}, device_id_type=MESH
        )
    pl.semaphore_wait(barrier, nx)

    def remote(src, dst, send, recv, target):
        return pltpu.make_async_remote_copy(
            src_ref=src, dst_ref=dst, send_sem=send, recv_sem=recv,
            device_id={"fs": fs, "tp": target}, device_id_type=MESH)

    def columns(t):
        return pl.ds(pl.multiple_of(t * width, width), width)

    parts = [pl.ds(i * step, step) for i in range(pieces)]
    offsets = list(range(1, nx)) + [0]
    sends = []
    for k in offsets:
        for i, part in enumerate(parts):
            copy = remote(partial.at[part, columns((x + k) % nx * 2 + (1 - core))], pair.at[k, part],
                          pair_send.at[k, i], pair_recv.at[k, i], partner)
            copy.start()
            sends.append(copy)
    for k in offsets[:-1]:
        target = (x + k) % nx * 2 + core
        for i, part in enumerate(parts):
            remote(pair.at[k, part], pair.at[k, part], pair_send.at[k, i], pair_recv.at[k, i], partner).wait_recv()
            pair_sum[k - 1, part] = (
                partial[part, columns(target)].astype(jnp.float32) + pair[k, part].astype(jnp.float32)
            ).astype(jnp.bfloat16)
            copy = remote(pair_sum.at[k - 1, part], cross.at[k - 1, part],
                          cross_send.at[k - 1, i], cross_recv.at[k - 1, i], target)
            copy.start()
            sends.append(copy)
    factor = 0.5 * scale[...]
    for i, part in enumerate(parts):
        remote(pair.at[0, part], pair.at[0, part], pair_send.at[0, i], pair_recv.at[0, i], partner).wait_recv()
        total = partial[part, columns(tp)].astype(jnp.float32) + pair[0, part].astype(jnp.float32)
        for k in range(1, nx):
            remote(cross.at[k - 1, part], cross.at[k - 1, part], cross_send.at[k - 1, i],
                   cross_recv.at[k - 1, i], partner).wait_recv()
            total = total + cross[k - 1, part].astype(jnp.float32)
        result = (resid[part].astype(jnp.float32) + total * factor).astype(jnp.bfloat16)
        if not gathers:
            out[part] = result
            continue
        out[tp, part] = result
        gather_send, gather_recv = sems[4:]
        for k in range(1, nx):
            copy = remote(out.at[tp, part], out.at[tp, part], gather_send.at[k - 1, i], gather_recv.at[tp, i],
                          (x + k) % nx * 2 + core)
            copy.start()
            sends.append(copy)
        copy = remote(out.at[tp, part], out.at[tp, part], gather_send.at[nx - 1, i], gather_recv.at[tp, i], partner)
        copy.start()
        sends.append(copy)
    if gathers:
        for k in range(1, nx):
            slot = (x + k) % nx * 2 + core
            for i, part in enumerate(parts):
                remote(out.at[slot, part], out.at[slot, part], gather_send.at[0, i], gather_recv.at[slot, i],
                       partner).wait_recv()
                copy = remote(out.at[slot, part], out.at[slot, part], gather_send.at[nx - 1 + k, i],
                              gather_recv.at[slot, i], partner)
                copy.start()
                sends.append(copy)
        for k in range(nx):
            slot = (x + k) % nx * 2 + (1 - core)
            for i, part in enumerate(parts):
                remote(out.at[slot, part], out.at[slot, part], gather_send.at[0, i], gather_recv.at[slot, i],
                       partner).wait_recv()
    for copy in sends:
        copy.wait_send()


def summed(ntp, gathers, identity, partial, resid, scale):
    nx = ntp // 2
    rows, width = resid.shape
    pieces = 3 if rows % 48 == 0 else 1
    vmem = pl.BlockSpec(memory_space=pltpu.VMEM)
    dma = pltpu.SemaphoreType.DMA
    scratch = [
        pltpu.VMEM((nx, rows, width), jnp.bfloat16),
        pltpu.VMEM((max(nx - 1, 1), rows, width), jnp.bfloat16),
        pltpu.VMEM((max(nx - 1, 1), rows, width), jnp.bfloat16),
        dma((nx, pieces)), dma((nx, pieces)), dma((nx, pieces)), dma((nx, pieces)),
    ]
    if gathers:
        scratch += [dma((2 * nx, pieces)), dma((ntp, pieces))]
    return pl.pallas_call(
        functools.partial(sum_kernel, ntp, gathers, pieces),
        name="sum_and_share" if gathers else "sum_last",
        out_shape=jax.ShapeDtypeStruct(((ntp,) if gathers else ()) + (rows, width), jnp.bfloat16),
        in_specs=[vmem] * 3,
        out_specs=vmem,
        scratch_shapes=scratch,
        compiler_params=pltpu.CompilerParams(
            collective_id=identity, has_side_effects=True, vmem_limit_bytes=32 << 20
        ),
    )(partial, resid, scale.reshape(1, width))


def joined(blocks):
    return jnp.swapaxes(blocks, 0, 1).reshape(blocks.shape[1], -1)


def rms(floats, norm_gain):
    scaled = floats * lax.rsqrt(jnp.mean(floats * floats, axis=-1, keepdims=True) + eps)
    return (scaled * norm_gain).astype(jnp.bfloat16)


def window_weights():
    position = jnp.arange(SEQ)
    rows, cols = position[:, None], position[None, :]
    mats = []
    for window in WINDOWS:
        low = jnp.maximum(rows - window // 2, 0)
        high = jnp.minimum(rows + window - window // 2, SEQ)
        mats.append(((cols >= low) & (cols < high)).astype(jnp.bfloat16))
    return mats


def pooling(pool_input):
    channels = pool_input.shape[1]
    group = channels // 4
    values = pool_input.reshape(-1, SEQ, channels)
    position = jnp.arange(SEQ)
    parts = []
    for index, (window, members) in enumerate(zip(WINDOWS, window_weights())):
        own = values[:, :, index * group:(index + 1) * group]
        sums = jnp.einsum("pq,sqc->spc", members, own, preferred_element_type=jnp.float32)
        before = window // 2
        counts = (
            jnp.minimum(position + window - before, SEQ) - jnp.maximum(position - before, 0)
        ).astype(jnp.float32)
        parts.append(sums / counts[None, :, None] - own.astype(jnp.float32))
    return jnp.concatenate(parts, axis=2).reshape(-1, channels).astype(jnp.bfloat16)


def body(
    nfs, ntp,
    stream, gain_first, gain_mixer, gain_second,
    gate_weight, gate_scale, up_weight, up_scale, down_weight, down_scale,
    pool_in_weight, pool_in_scale, pool_out_weight, pool_out_scale,
):
    half = jnp.bfloat16
    in_half, out_half = pool_in_weight.astype(half), pool_out_weight.astype(half)
    in_rows, in_cols = in_half.shape
    out_rows, out_cols = out_half.shape
    pool = jnp.concatenate([in_half, out_half.reshape(-1, in_cols)], axis=0)
    pool_all, gate_all, up_all, down_all, stream_all = gather_all(
        nfs, ntp, pool, gate_weight.astype(half), up_weight.astype(half), down_weight.astype(half), stream
    )
    in_whole = pool_all[:, :, :in_rows].transpose(1, 2, 0, 3).reshape(nfs * in_rows, ntp * in_cols)
    out_whole = (
        pool_all[:, :, in_rows:].reshape(ntp, nfs, out_rows, out_cols)
        .transpose(0, 2, 1, 3).reshape(ntp * out_rows, nfs * out_cols)
    )
    gate_whole = gate_all.reshape(-1, gate_all.shape[-1])
    up_whole = up_all.reshape(-1, up_all.shape[-1])
    down_whole = jnp.swapaxes(down_all, 0, 1).reshape(down_all.shape[1], -1)
    in_scale = lax.all_gather(pool_in_scale, "tp", tiled=True)
    out_scale = lax.all_gather(pool_out_scale, "tp", tiled=True)
    tp = lax.axis_index("tp")

    def feed_forward(rows):
        gate_sum = jnp.dot(rows, gate_whole, preferred_element_type=jnp.float32) * gate_scale
        up_sum = jnp.dot(rows, up_whole, preferred_element_type=jnp.float32) * up_scale
        hidden = (jax.nn.silu(gate_sum) * up_sum).astype(half)
        return jnp.dot(hidden, down_whole, preferred_element_type=jnp.float32).astype(half)

    first = rms(joined(stream_all).astype(jnp.float32), gain_first)
    after_first = joined(summed(ntp, True, 1, feed_forward(first), stream, down_scale))
    mixer_normed = rms(after_first.astype(jnp.float32), gain_mixer)
    pool_input = (
        jnp.dot(mixer_normed, in_whole, preferred_element_type=jnp.float32) * in_scale
    ).astype(half)
    mixed = jnp.dot(pooling(pool_input), out_whole, preferred_element_type=jnp.float32)
    after_mix = (after_first.astype(jnp.float32) + mixed * out_scale).astype(half)
    second = rms(after_mix.astype(jnp.float32), gain_second)
    own = lax.dynamic_slice_in_dim(after_mix, tp * stream.shape[1], stream.shape[1], axis=1)
    return summed(ntp, False, 2, feed_forward(second), own, down_scale)


def solution(mesh):
    placed = (
        P("fs", "tp"), P(), P(), P(),
        P("fs", "tp"), P("tp"), P("fs", "tp"), P("tp"), P("tp", "fs"), P("tp"),
        P("fs", "tp"), P("tp"), P("tp", "fs"), P("tp"),
    )
    return jax.shard_map(
        functools.partial(body, mesh.shape["fs"], mesh.shape["tp"]),
        mesh=mesh, in_specs=placed, out_specs=P("fs", "tp"), check_vma=False,
    )
```

```python
import functools

import jax
import jax.numpy as jnp
from jax import lax
from jax.experimental import pallas as pl
from jax.experimental.pallas import tpu as pltpu
from jax.sharding import PartitionSpec as P

SEQ = 128
MESH = pl.DeviceIdType.MESH

eps = 1e-06
WINDOWS = (2, 4, 8, 16)


def fs_grid(count):
    ny = 1
    while (2 * ny) * (2 * ny) <= count and count % (2 * ny) == 0:
        ny *= 2
    return ny, count // ny


def grid_shape(row_blocks, col_blocks, block):
    rows, cols = block
    if cols % 128 == 0:
        return (row_blocks * rows, col_blocks * cols)
    return (row_blocks, col_blocks, rows, cols)


def place(whole, block, row_block, col_block, part=(0, None)):
    rows, cols = block
    first, count = part[0], rows if part[1] is None else part[1]
    if len(whole.shape) == 2:
        return whole.at[
            pl.ds(pl.multiple_of(row_block * rows + first, 16), count),
            pl.ds(pl.multiple_of(col_block * cols, 128), cols),
        ]
    return whole.at[row_block, col_block, pl.ds(first, count)]


def flat(whole):
    if whole.ndim == 2:
        return whole
    return whole.transpose(0, 2, 1, 3).reshape(whole.shape[0] * whole.shape[2], -1)


def gather_kernel(nfs, ntp, pool_in, pool_out, gate, up, down, stream, scales,
                  in_all, out_all, gate_all, up_all, down_all, stream_all, scales_all,
                  send_sem, recv_sem, local_sem, tsend, trecv, psend, precv, ssend, srecv):
    ny, nz = fs_grid(nfs)
    nx = ntp // 2
    fs, tp = lax.axis_index("fs"), lax.axis_index("tp")
    z, y = fs // ny, fs % ny
    x, core = tp // 2, tp % 2
    partner = x * 2 + (1 - core)
    alternate = ny == 2 and nz > 1

    barrier = pltpu.get_barrier_semaphore()

    def greet(cond, f, t):
        @pl.when(cond)
        def _():
            pl.semaphore_signal(barrier, inc=1, device_id={"fs": f, "tp": t}, device_id_type=MESH)

    greet(z > 0, fs - ny, tp)
    greet(z < nz - 1, fs + ny, tp)
    greet(y > 0, fs - 1, tp)
    greet(y < ny - 1, fs + 1, tp)
    for k in range(1, ntp):
        pl.semaphore_signal(
            barrier, inc=1, device_id={"fs": fs, "tp": (tp + k) % ntp}, device_id_type=MESH
        )
    peers = ntp - 1
    for cond in (z > 0, z < nz - 1, y > 0, y < ny - 1):
        peers = peers + jnp.where(cond, 1, 0)
    pl.semaphore_wait(barrier, peers)

    pieces = [
        (lambda: pool_in, lambda f: place(in_all, pool_in.shape, f, tp)),
        (lambda: pool_out, lambda f: place(out_all, pool_out.shape, tp, f)),
    ]
    npool = len(pieces)
    for own, whole, by_rows in ((gate, gate_all, True), (up, up_all, True), (down, down_all, False)):
        rows = own.shape[0]
        halves = 2 if alternate else 1
        for h in range(halves):
            part = (h * (rows // halves), rows // halves)

            def own_part(own=own, part=part):
                return own.at[pl.ds(*part)]

            def whole_part(f, own=own, whole=whole, part=part, by_rows=by_rows):
                return place(whole, own.shape, f if by_rows else 0, 0 if by_rows else f, part)

            pieces.append((own_part, whole_part))
    started = []

    def remote(piece, f, direction, target, mine=False):
        own, whole = pieces[piece]
        return pltpu.make_async_remote_copy(
            src_ref=own() if mine else whole(f),
            dst_ref=whole(f),
            send_sem=send_sem.at[piece, f, direction],
            recv_sem=recv_sem.at[piece, f],
            device_id={"fs": target, "tp": tp},
            device_id_type=MESH,
        )

    def send(cond, piece, f, direction, mine=False):
        target = fs + (-ny, ny, -1, 1)[direction]

        @pl.when(cond)
        def _():
            remote(piece, f, direction, target, mine).start()

        started.append((cond, piece, f, direction, target, mine))

    def arrived(cond, piece, f):
        @pl.when(cond)
        def _():
            remote(piece, f, 0, fs, False).wait_recv()

    def by_y(cond, piece, f, mine=False):
        send(cond & (y > 0), piece, f, 2, mine)
        send(cond & (y < ny - 1), piece, f, 3, mine)

    yes = z >= 0

    def stream_place(slot):
        return place(stream_all, stream.shape, 0, slot)

    def stream_copy(src, slot, t_target, k):
        return pltpu.make_async_remote_copy(
            src_ref=src, dst_ref=stream_place(slot), send_sem=tsend.at[k], recv_sem=trecv.at[slot],
            device_id={"fs": fs, "tp": t_target}, device_id_type=MESH)

    def slab(which, slot):
        if which == 0:
            if len(in_all.shape) == 2:
                cols = pool_in.shape[1]
                return in_all.at[:, pl.ds(pl.multiple_of(slot * cols, 128), cols)]
            return in_all.at[:, slot]
        if len(out_all.shape) == 2:
            rows = pool_out.shape[0]
            return out_all.at[pl.ds(pl.multiple_of(slot * rows, 16), rows)]
        return out_all.at[slot]

    def pool_copy(which, slot, t_target, k):
        return pltpu.make_async_remote_copy(
            src_ref=slab(which, slot), dst_ref=slab(which, slot),
            send_sem=psend.at[which, k], recv_sem=precv.at[which, slot],
            device_id={"fs": fs, "tp": t_target}, device_id_type=MESH)

    def scale_copy(k, slot, t_target):
        return pltpu.make_async_remote_copy(
            src_ref=scales, dst_ref=scales_all.at[slot], send_sem=ssend.at[k], recv_sem=srecv.at[slot],
            device_id={"fs": fs, "tp": t_target}, device_id_type=MESH)

    npieces = len(pieces)
    locals_ = [pltpu.make_async_copy(own(), whole(fs), local_sem.at[i]) for i, (own, whole) in enumerate(pieces)]
    locals_.append(pltpu.make_async_copy(stream, stream_place(tp), local_sem.at[npieces]))
    locals_.append(pltpu.make_async_copy(scales, scales_all.at[tp], local_sem.at[npieces + 1]))
    for piece in range(npieces):
        send(z > 0, piece, fs, 0, True)
        send(z < nz - 1, piece, fs, 1, True)
        by_y(yes, piece, fs, True)
    stream_sends = []
    for k in range(1, nx):
        stream_sends.append(stream_copy(stream, tp, (x + k) % nx * 2 + core, k - 1))
    stream_sends.append(stream_copy(stream, tp, partner, nx - 1))
    stream_sends += [scale_copy(k - 1, tp, (tp + k) % ntp) for k in range(1, ntp)]
    for copy in stream_sends:
        copy.start()
    for copy in locals_:
        copy.start()

    def row_arrivals(piece, d, alt):
        low, high = fs - d * ny, fs + d * ny
        has_low, has_high = z >= d, z + d <= nz - 1
        for cond, f, direction, ahead, end in (
            (has_low, low, 1, z < nz - 1, z == d),
            (has_high, high, 0, z > 0, z + d == nz - 1),
        ):
            arrived(cond, piece, f)
            send(cond & ahead, piece, f, direction)
            if alt:
                by_y(cond & jnp.logical_not(end), piece, f)
                other = f + 1 - 2 * y
                arrived(cond & end, piece, other)
                send(cond & end & ahead, piece, other, direction)
            else:
                by_y(cond, piece, f)

    def column_arrivals(piece, alt):
        for d in range(nz):
            for sign in ((1,) if d == 0 else (-1, 1)):
                row_ok = (z + sign * d >= 0) & (z + sign * d <= nz - 1)
                if alt:
                    at = z + sign * d
                    if d == 0:
                        continue
                    row_ok = row_ok & (at != 0) & (at != nz - 1)
                base = fs + sign * d * ny
                for e in range(1, ny):
                    for step, direction, ok, ahead in (
                        (-e, 3, y >= e, y < ny - 1),
                        (e, 2, y + e <= ny - 1, y > 0),
                    ):
                        arrived(row_ok & ok, piece, base + step)
                        if ny > 2:
                            send(row_ok & ok & ahead, piece, base + step, direction)

    is_alt = [alternate and p >= npool and p % 2 == 1 for p in range(npieces)]

    for d in range(1, nz):
        for p in range(npool):
            row_arrivals(p, d, False)
    pool_sends = []
    for p in range(npool):
        column_arrivals(p, False)
        locals_[p].wait()
        pool_sends += [pool_copy(p, tp, (x + k) % nx * 2 + core, k - 1) for k in range(1, nx)]
        pool_sends.append(pool_copy(p, tp, partner, nx - 1))
    for copy in pool_sends:
        copy.start()
    for k in range(1, nx):
        slot = (x + k) % nx * 2 + core
        stream_copy(stream, slot, partner, 0).wait_recv()
        copy = stream_copy(stream_place(slot), slot, partner, nx - 1 + k)
        copy.start()
        stream_sends.append(copy)

    for p in range(npieces):
        if is_alt[p]:
            other = fs + 1 - 2 * y
            arrived(yes, p, other)
            send(z == 0, p, other, 1)
            send(z == nz - 1, p, other, 0)
    for d in range(1, nz):
        for p in range(npool, npieces):
            row_arrivals(p, d, is_alt[p])
        if d == 1:
            for k in range(1, nx):
                slot = (x + k) % nx * 2 + core
                for p in range(npool):
                    pool_copy(p, slot, partner, 0).wait_recv()
                    copy = pool_copy(p, slot, partner, nx - 1 + k)
                    copy.start()
                    pool_sends.append(copy)
    for p in range(npool, npieces):
        column_arrivals(p, is_alt[p])
    for k in range(nx):
        slot = (x + k) % nx * 2 + (1 - core)
        stream_copy(stream, slot, partner, 0).wait_recv()
        for p in range(npool):
            pool_copy(p, slot, partner, 0).wait_recv()
    for k in range(1, ntp):
        scale_copy(0, (tp + k) % ntp, partner).wait_recv()
    for copy in locals_[npool:]:
        copy.wait()
    for copy in stream_sends + pool_sends:
        copy.wait_send()
    for cond, piece, f, direction, target, mine in started:
        @pl.when(cond)
        def _():
            remote(piece, f, direction, target, mine).wait_send()


def gather_all(nfs, ntp, pool_in, pool_out, gate, up, down, stream, scales):
    ny, nz = fs_grid(nfs)
    nx = ntp // 2
    npieces = 8 if (ny == 2 and nz > 1) else 5
    any_spec = pl.BlockSpec(memory_space=pl.ANY)
    shapes = (
        grid_shape(nfs, ntp, pool_in.shape),
        grid_shape(ntp, nfs, pool_out.shape),
        grid_shape(nfs, 1, gate.shape),
        grid_shape(nfs, 1, up.shape),
        grid_shape(1, nfs, down.shape),
        grid_shape(1, ntp, stream.shape),
    )
    dma = pltpu.SemaphoreType.DMA
    return pl.pallas_call(
        functools.partial(gather_kernel, nfs, ntp),
        name="collect_weights",
        out_shape=tuple(jax.ShapeDtypeStruct(shape, jnp.bfloat16) for shape in shapes)
        + (jax.ShapeDtypeStruct((ntp,) + scales.shape, jnp.float32),),
        in_specs=[any_spec] * 7,
        out_specs=[any_spec] * 7,
        scratch_shapes=[
            dma((npieces, nfs, 4)),
            dma((npieces, nfs)),
            dma((npieces + 2,)),
            dma((2 * nx,)),
            dma((ntp,)),
            dma((2, 2 * nx)),
            dma((2, ntp)),
            dma((ntp,)),
            dma((ntp,)),
        ],
        compiler_params=pltpu.CompilerParams(collective_id=0, has_side_effects=True, vmem_limit_bytes=1 << 20),
    )(pool_in, pool_out, gate, up, down, stream, scales)


def sum_kernel(ntp, gathers, pieces, partial, resid, scale, out, pair, pair_sum, cross, *sems):
    pair_send, pair_recv, cross_send, cross_recv = sems[:4]
    nx = ntp // 2
    tp, fs = lax.axis_index("tp"), lax.axis_index("fs")
    x, core = tp // 2, tp % 2
    partner = x * 2 + (1 - core)
    rows, width = resid.shape
    step = rows // pieces
    barrier = pltpu.get_barrier_semaphore()
    pl.semaphore_signal(barrier, inc=1, device_id={"fs": fs, "tp": partner}, device_id_type=MESH)
    for k in range(1, nx):
        pl.semaphore_signal(
            barrier, inc=1, device_id={"fs": fs, "tp": (x + k) % nx * 2 + core}, device_id_type=MESH
        )
    pl.semaphore_wait(barrier, nx)

    def remote(src, dst, send, recv, target):
        return pltpu.make_async_remote_copy(
            src_ref=src, dst_ref=dst, send_sem=send, recv_sem=recv,
            device_id={"fs": fs, "tp": target}, device_id_type=MESH)

    def columns(t):
        return pl.ds(pl.multiple_of(t * width, width), width)

    parts = [pl.ds(i * step, step) for i in range(pieces)]
    offsets = list(range(1, nx)) + [0]
    sends = []
    for k in offsets:
        for i, part in enumerate(parts):
            copy = remote(partial.at[part, columns((x + k) % nx * 2 + (1 - core))], pair.at[k, part],
                          pair_send.at[k, i], pair_recv.at[k, i], partner)
            copy.start()
            sends.append(copy)
    for k in offsets[:-1]:
        target = (x + k) % nx * 2 + core
        for i, part in enumerate(parts):
            remote(pair.at[k, part], pair.at[k, part], pair_send.at[k, i], pair_recv.at[k, i], partner).wait_recv()
            pair_sum[k - 1, part] = (
                partial[part, columns(target)].astype(jnp.float32) + pair[k, part].astype(jnp.float32)
            ).astype(jnp.bfloat16)
            copy = remote(pair_sum.at[k - 1, part], cross.at[k - 1, part],
                          cross_send.at[k - 1, i], cross_recv.at[k - 1, i], target)
            copy.start()
            sends.append(copy)
    factor = 0.5 * scale[...]
    for i, part in enumerate(parts):
        remote(pair.at[0, part], pair.at[0, part], pair_send.at[0, i], pair_recv.at[0, i], partner).wait_recv()
        total = partial[part, columns(tp)].astype(jnp.float32) + pair[0, part].astype(jnp.float32)
        for k in range(1, nx):
            remote(cross.at[k - 1, part], cross.at[k - 1, part], cross_send.at[k - 1, i],
                   cross_recv.at[k - 1, i], partner).wait_recv()
            total = total + cross[k - 1, part].astype(jnp.float32)
        result = (resid[part].astype(jnp.float32) + total * factor).astype(jnp.bfloat16)
        if not gathers:
            out[part] = result
            continue
        out[part, columns(tp)] = result
        gather_send, gather_recv = sems[4:]
        for k in range(1, nx):
            copy = remote(out.at[part, columns(tp)], out.at[part, columns(tp)], gather_send.at[k - 1, i], gather_recv.at[tp, i],
                          (x + k) % nx * 2 + core)
            copy.start()
            sends.append(copy)
        copy = remote(out.at[part, columns(tp)], out.at[part, columns(tp)], gather_send.at[nx - 1, i], gather_recv.at[tp, i], partner)
        copy.start()
        sends.append(copy)
    if gathers:
        for k in range(1, nx):
            slot = (x + k) % nx * 2 + core
            for i, part in enumerate(parts):
                remote(out.at[part, columns(slot)], out.at[part, columns(slot)], gather_send.at[0, i], gather_recv.at[slot, i],
                       partner).wait_recv()
                copy = remote(out.at[part, columns(slot)], out.at[part, columns(slot)], gather_send.at[nx - 1 + k, i],
                              gather_recv.at[slot, i], partner)
                copy.start()
                sends.append(copy)
        for k in range(nx):
            slot = (x + k) % nx * 2 + (1 - core)
            for i, part in enumerate(parts):
                remote(out.at[part, columns(slot)], out.at[part, columns(slot)], gather_send.at[0, i], gather_recv.at[slot, i],
                       partner).wait_recv()
    for copy in sends:
        copy.wait_send()


def summed(ntp, gathers, identity, partial, resid, scale):
    nx = ntp // 2
    rows, width = resid.shape
    pieces = 3 if rows % 48 == 0 else 1
    vmem = pl.BlockSpec(memory_space=pltpu.VMEM)
    dma = pltpu.SemaphoreType.DMA
    scratch = [
        pltpu.VMEM((nx, rows, width), jnp.bfloat16),
        pltpu.VMEM((max(nx - 1, 1), rows, width), jnp.bfloat16),
        pltpu.VMEM((max(nx - 1, 1), rows, width), jnp.bfloat16),
        dma((nx, pieces)), dma((nx, pieces)), dma((nx, pieces)), dma((nx, pieces)),
    ]
    if gathers:
        scratch += [dma((2 * nx, pieces)), dma((ntp, pieces))]
    return pl.pallas_call(
        functools.partial(sum_kernel, ntp, gathers, pieces),
        name="sum_and_share" if gathers else "sum_last",
        out_shape=jax.ShapeDtypeStruct((rows, width * (ntp if gathers else 1)), jnp.bfloat16),
        in_specs=[vmem] * 3,
        out_specs=vmem,
        scratch_shapes=scratch,
        compiler_params=pltpu.CompilerParams(
            collective_id=identity, has_side_effects=True, vmem_limit_bytes=32 << 20
        ),
    )(partial, resid, scale.reshape(1, width))


def rms(floats, norm_gain):
    scaled = floats * lax.rsqrt(jnp.mean(floats * floats, axis=-1, keepdims=True) + eps)
    return (scaled * norm_gain).astype(jnp.bfloat16)


def window_weights():
    position = jnp.arange(SEQ)
    rows, cols = position[:, None], position[None, :]
    mats = []
    for window in WINDOWS:
        low = jnp.maximum(rows - window // 2, 0)
        high = jnp.minimum(rows + window - window // 2, SEQ)
        mats.append(((cols >= low) & (cols < high)).astype(jnp.bfloat16))
    return mats


def pooling(pool_input):
    channels = pool_input.shape[1]
    group = channels // 4
    values = pool_input.reshape(-1, SEQ, channels)
    position = jnp.arange(SEQ)
    parts = []
    for index, (window, members) in enumerate(zip(WINDOWS, window_weights())):
        own = values[:, :, index * group:(index + 1) * group]
        sums = jnp.einsum("pq,sqc->spc", members, own, preferred_element_type=jnp.float32)
        before = window // 2
        counts = (
            jnp.minimum(position + window - before, SEQ) - jnp.maximum(position - before, 0)
        ).astype(jnp.float32)
        parts.append(sums / counts[None, :, None] - own.astype(jnp.float32))
    return jnp.concatenate(parts, axis=2).reshape(-1, channels).astype(jnp.bfloat16)


def body(
    nfs, ntp,
    stream, gain_first, gain_mixer, gain_second,
    gate_weight, gate_scale, up_weight, up_scale, down_weight, down_scale,
    pool_in_weight, pool_in_scale, pool_out_weight, pool_out_scale,
):
    half = jnp.bfloat16
    in_half, out_half = pool_in_weight.astype(half), pool_out_weight.astype(half)
    width, channels = stream.shape[1], in_half.shape[1]
    scales = jnp.concatenate([pool_in_scale, pool_out_scale]).reshape(1, -1)
    in_all, out_all, gate_all, up_all, down_all, stream_all, scales_all = gather_all(
        nfs, ntp, in_half, out_half, gate_weight.astype(half), up_weight.astype(half), down_weight.astype(half),
        stream, scales,
    )
    in_whole, out_whole = flat(in_all), flat(out_all)
    gate_whole, up_whole, down_whole = flat(gate_all), flat(up_all), flat(down_all)
    in_scale = scales_all[:, 0, :channels].reshape(-1)
    out_scale = scales_all[:, 0, channels:].reshape(-1)
    tp = lax.axis_index("tp")

    def feed_forward(rows):
        gate_sum = jnp.dot(rows, gate_whole, preferred_element_type=jnp.float32) * gate_scale
        up_sum = jnp.dot(rows, up_whole, preferred_element_type=jnp.float32) * up_scale
        hidden = (jax.nn.silu(gate_sum) * up_sum).astype(half)
        return jnp.dot(hidden, down_whole, preferred_element_type=jnp.float32).astype(half)

    first = rms(flat(stream_all).astype(jnp.float32), gain_first)
    after_first = summed(ntp, True, 1, feed_forward(first), stream, down_scale)
    mixer_normed = rms(after_first.astype(jnp.float32), gain_mixer)
    pool_input = (
        jnp.dot(mixer_normed, in_whole, preferred_element_type=jnp.float32) * in_scale
    ).astype(half)
    mixed = jnp.dot(pooling(pool_input), out_whole, preferred_element_type=jnp.float32)
    after_mix = (after_first.astype(jnp.float32) + mixed * out_scale).astype(half)
    second = rms(after_mix.astype(jnp.float32), gain_second)
    own = lax.dynamic_slice_in_dim(after_mix, tp * stream.shape[1], stream.shape[1], axis=1)
    return summed(ntp, False, 2, feed_forward(second), own, down_scale)


def solution(mesh):
    placed = (
        P("fs", "tp"), P(), P(), P(),
        P("fs", "tp"), P("tp"), P("fs", "tp"), P("tp"), P("tp", "fs"), P("tp"),
        P("fs", "tp"), P("tp"), P("tp", "fs"), P("tp"),
    )
    return jax.shard_map(
        functools.partial(body, mesh.shape["fs"], mesh.shape["tp"]),
        mesh=mesh, in_specs=placed, out_specs=P("fs", "tp"), check_vma=False,
    )
```
